32 devices in a mesh: rep: 2 (over y), fs: 4 (over z), tp: 4 (over x, core).
Axes of the slice: x: 2, y: 2, z: 4, core: 2. Of those that a mesh axis runs over, the one named last changes fastest.
Arguments:
- tokens: bfloat16 [2048, 2048], P(('rep', 'fs')), may hold values from -6 to 6
- gate_weight: bfloat16 [2048, 2816], P('fs', 'tp'), may hold values from -0.125 to 0.125
- up_weight: bfloat16 [2048, 2816], P('fs', 'tp'), may hold values from -0.125 to 0.125
- down_weight: bfloat16 [2816, 2048], P('tp', 'fs'), may hold values from -0.109375 to 0.109375
- out_grad: bfloat16 [2048, 2048], P(('rep', 'fs')), may hold values from -6 to 6
Outputs:
- input_grad: bfloat16 [2048, 2048], P(('rep', 'fs'))
- down_grad: float32 [2816, 2048], P('tp', 'fs')
- row_norms: float32 [2816], P('tp')
The draws below stay inside these ranges and needn't reach their ends.
All inputs are finite; a program needn't handle non-finite values.
Results may differ from the reference program's by a relative error of at most 0.024.
Values may be sent and summed in bfloat16 or wider, within the bound.
A program may use at most 64 MiB of HBM per device.

```python
import jax
import jax.numpy as jnp
from jax import lax

D = 2048
FF = 2816
TOKENS = 2048
N_TP = 4


def spiked(drawn, rng, source, target, parts, factor):
    def block_of(axis_at):
        return (jnp.arange(drawn.shape[axis_at]) // (drawn.shape[axis_at] // parts)).reshape((-1,) + (1,) * (drawn.ndim - 1 - axis_at))

    first = jax.random.permutation(rng, parts)[block_of(target)]
    second = (block_of(target) + parts // 2) % parts
    return jnp.where((block_of(source) == first) | (block_of(source) == second), factor * drawn, drawn)


def steps_of(own_key, dims, split, least, largest):
    def one(dim, blocks):
        steps = jax.random.uniform(jax.random.fold_in(jax.random.fold_in(own_key, 6), dim), (blocks,), jnp.float32, least / len(split), largest / len(split))
        return jnp.repeat(jnp.exp(steps), dims[dim] // blocks).reshape((-1,) + (1,) * (len(dims) - dim - 1))

    loudness = one(*split[0])
    for cut in split[1:]:
        loudness = loudness * one(*cut)
    return loudness


def noise(stream_key, extent, width, most, pieces=(), kind=jnp.bfloat16):
    entries = jax.random.normal(stream_key, extent, jnp.float32) * width
    if len(pieces) > 0:
        entries = steps_of(stream_key, extent, pieces, -0.22, 0.18) * entries
    return jnp.clip(entries, min=-most, max=most).astype(kind)


def noise_with(rng, dims, scale, bound, cuts, heavy, held_as=jnp.bfloat16):
    drawn = scale * jax.random.normal(rng, dims, jnp.float32)
    if cuts:
        drawn = drawn * steps_of(rng, dims, cuts, -0.22, 0.18)
    return jnp.clip(spiked(drawn, jax.random.fold_in(rng, 3), *heavy), -bound, bound).astype(held_as)


def setup_inputs(seed: int = 0) -> dict:
    key_of = jax.random.split(jax.random.key(seed), 6)
    tokens = noise(key_of[0], (TOKENS, D), 1.0, 6.0, ((0, 8),))
    gate_weight = noise(key_of[1], (D, FF), D ** -0.5, 0.125, ((0, 4), (1, 4)))
    up_weight = noise(key_of[2], (D, FF), D ** -0.5, 0.125, ((0, 4), (1, 4)))
    down_weight = noise(key_of[3], (FF, D), FF ** -0.5, 0.109375, ((0, 4), (1, 4)))
    out_grad = noise_with(key_of[4], (TOKENS, D), 1.0, 6.0, ((0, 8),), (0, 1, 8, 2.0))
    return {"tokens": tokens, "gate_weight": gate_weight, "up_weight": up_weight, "down_weight": down_weight, "out_grad": out_grad}


def reference(tokens, gate_weight, up_weight, down_weight, out_grad):
    gate_pre = jnp.dot(tokens, gate_weight, preferred_element_type=jnp.float32)
    up_pre = jnp.dot(tokens, up_weight, preferred_element_type=jnp.float32)
    sigma = jax.nn.sigmoid(gate_pre)
    activated = gate_pre * sigma
    hidden = (activated * up_pre).astype(jnp.bfloat16)
    hid_grad = lax.dot_general(out_grad, down_weight, (((1,), (1,)), ((), ())), preferred_element_type=jnp.float32)
    up_grad = (hid_grad * activated).astype(jnp.bfloat16)
    gate_grad = (hid_grad * up_pre * sigma * (1.0 + gate_pre * (1.0 - sigma))).astype(jnp.bfloat16)
    block = FF // N_TP

    def add_block(index, total):
        offset = (index * block).astype(jnp.int32)
        gate_part = lax.dynamic_slice_in_dim(gate_grad, offset, block, 1)
        up_part = lax.dynamic_slice_in_dim(up_grad, offset, block, 1)
        gate_rows = lax.dynamic_slice_in_dim(gate_weight, offset, block, 1)
        up_rows = lax.dynamic_slice_in_dim(up_weight, offset, block, 1)
        partial_value = lax.dot_general(gate_part, gate_rows, (((1,), (1,)), ((), ())), preferred_element_type=jnp.float32)
        partial_value = partial_value + lax.dot_general(up_part, up_rows, (((1,), (1,)), ((), ())), preferred_element_type=jnp.float32)
        return total + partial_value.astype(jnp.bfloat16).astype(jnp.float32)

    total = lax.fori_loop(0, N_TP, add_block, jnp.zeros(tokens.shape, jnp.float32))
    input_grad = total.astype(jnp.bfloat16)
    down_grad = lax.dot_general(hidden, out_grad, (((0,), (0,)), ((), ())), preferred_element_type=jnp.float32)
    row_norms = jnp.sum(down_grad * down_grad, axis=1)
    return input_grad, down_grad, row_norms
```

```python
import functools

import jax
import jax.numpy as jnp
from jax import lax
from jax.experimental import pallas as pl
from jax.experimental.pallas import tpu as pltpu
from jax.sharding import PartitionSpec as P

MESH = pl.DeviceIdType.MESH
BF16 = jnp.bfloat16
F32 = jnp.float32


def contract_last(left, right):
    return lax.dot_general(left, right, (((1,), (1,)), ((), ())), preferred_element_type=F32)


def contract_first(left, right):
    return lax.dot_general(left, right, (((0,), (0,)), ((), ())), preferred_element_type=F32)


def gather_kernel(
    n, gate, up, down, tokens, grad, gate_all, up_all, down_all, tokens_all, grad_all,
    right_send, right_recv, left_send, left_recv, pair_send, pair_recv, own_sem,
):
    f = lax.axis_index("fs")
    r = lax.axis_index("rep")
    rows, width = tokens.shape[0], gate.shape[1]
    other = 1 - r

    barrier = pltpu.get_barrier_semaphore()
    for k in range(1, n):
        pl.semaphore_signal(barrier, inc=1, device_id={"fs": lax.rem(f + k, n)}, device_id_type=MESH)
    pl.semaphore_signal(barrier, inc=1, device_id={"rep": other}, device_id_type=MESH)
    pl.semaphore_wait(barrier, n)

    shards = ((gate, gate_all), (up, up_all), (down, down_all))

    def columns(owner):
        return pl.ds(pl.multiple_of(owner * width, width), width)

    def hop(w, step, right):
        own, whole = shards[w]
        owner = f - step if right else f + step
        place = whole.at[:, columns(owner)]
        return pltpu.make_async_remote_copy(
            src_ref=own if step == 0 else place,
            dst_ref=place,
            send_sem=(right_send if right else left_send).at[w, step],
            recv_sem=(right_recv if right else left_recv).at[w, step],
            device_id={"fs": f + 1 if right else f - 1},
            device_id_type=MESH,
        )

    def arrival(w, step, right):
        own, whole = shards[w]
        owner = f - 1 - step if right else f + 1 + step
        place = whole.at[:, columns(owner)]
        return pltpu.make_async_remote_copy(
            src_ref=place,
            dst_ref=place,
            send_sem=(right_send if right else left_send).at[w, step],
            recv_sem=(right_recv if right else left_recv).at[w, step],
            device_id={"fs": f - 1 if right else f + 1},
            device_id_type=MESH,
        )

    def sends(step, right):
        return (f < n - 1) & (f >= step) if right else (f > 0) & (f + step <= n - 1)

    def receives(step, right):
        return f - 1 - step >= 0 if right else f + 1 + step <= n - 1

    for w in range(3):
        for right in (True, False):
            @pl.when(sends(0, right))
            def _():
                hop(w, 0, right).start()

    pairs = []
    for i, (own, whole) in enumerate(((tokens, tokens_all), (grad, grad_all))):
        copy = pltpu.make_async_remote_copy(
            src_ref=own, dst_ref=whole.at[pl.ds(rows, rows)],
            send_sem=pair_send.at[i], recv_sem=pair_recv.at[i],
            device_id={"rep": other}, device_id_type=MESH,
        )
        copy.start()
        pairs.append(copy)
    local = []
    for i, (own, place) in enumerate((
        (tokens, tokens_all.at[pl.ds(0, rows)]),
        (grad, grad_all.at[pl.ds(0, rows)]),
        (gate, gate_all.at[:, columns(f)]),
        (up, up_all.at[:, columns(f)]),
        (down, down_all.at[:, columns(f)]),
    )):
        copy = pltpu.make_async_copy(own, place, own_sem.at[i])
        copy.start()
        local.append(copy)

    for step in range(n - 1):
        for w in range(3):
            for right in (True, False):
                @pl.when(receives(step, right))
                def _():
                    arrival(w, step, right).wait_recv()
                if step + 1 < n - 1:
                    @pl.when(sends(step + 1, right))
                    def _():
                        hop(w, step + 1, right).start()
    for step in range(n - 1):
        for w in range(3):
            for right in (True, False):
                @pl.when(sends(step, right))
                def _():
                    hop(w, step, right).wait_send()
    for copy in pairs:
        copy.wait()
    for copy in local:
        copy.wait()


def reduce_kernel(
    n, part, flow, input_grad, down_grad, norms,
    p_in, g_core, g_sum, g_rep, g_half, g_x, g_out, s_own, s_other, n_own, n_in,
    p_send, p_recv, g_send, g_recv, s_send, s_recv, n_send, n_recv,
):
    f = lax.axis_index("fs")
    r = lax.axis_index("rep")
    t = lax.axis_index("tp")
    c, x = lax.rem(t, 2), t // 2
    mate, far = x * 2 + 1 - c, (1 - x) * 2 + c
    units, width = p_in.shape[1], p_in.shape[2]
    rows = input_grad.shape[0]
    half, quarter = flow.shape[1] // 2, flow.shape[1] // 4

    barrier = pltpu.get_barrier_semaphore()
    peers = [{"rep": lax.rem(r + a, 2), "fs": lax.rem(f + k, n)}
             for a in range(2) for k in range(n) if a or k]
    for peer in peers + [{"tp": mate}, {"tp": far}]:
        pl.semaphore_signal(barrier, inc=1, device_id=peer, device_id_type=MESH)
    pl.semaphore_wait(barrier, 2 * n + 1)

    def cols(start, size):
        return pl.ds(pl.multiple_of(start, size), size)

    def push(i, src, dst, peer):
        copy = pltpu.make_async_remote_copy(
            src_ref=src, dst_ref=dst, send_sem=g_send.at[i], recv_sem=g_recv.at[i],
            device_id=peer, device_id_type=MESH,
        )
        copy.start()
        return copy

    first = push(0, flow.at[:, cols((1 - c) * half, half)], g_core, {"tp": mate})
    shards = []
    for k in range(1, n):
        to = lax.rem(f + k, n)
        copy = pltpu.make_async_remote_copy(
            src_ref=part.at[:, cols(to * width, width)], dst_ref=p_in.at[k - 1],
            send_sem=p_send.at[k - 1], recv_sem=p_recv.at[k - 1],
            device_id={"fs": to}, device_id_type=MESH,
        )
        copy.start()
        shards.append(copy)

    first.wait()
    for b in (1, 0):
        span = pl.ds(b * rows, rows)
        g_sum[b] = (flow[span, cols(c * half, half)].astype(F32) + g_core[span].astype(F32)).astype(BF16)
        if b == 1:
            second = push(1, g_sum.at[1], g_rep, {"rep": 1 - r})
    second.wait()
    for b in range(2):
        at = pl.ds(b * quarter, quarter)
        g_half[b] = (g_sum[0, :, at].astype(F32) + g_rep[:, at].astype(F32)).astype(BF16)
    third = push(2, g_half.at[1 - x], g_x, {"tp": far})
    third.wait()
    mine = cols(c * half + x * quarter, quarter)
    g_out[:, mine] = (g_half[x].astype(F32) + g_x[...].astype(F32)).astype(BF16)
    fourth = push(3, g_out.at[:, mine], g_out.at[:, mine], {"tp": far})

    total = part[:, cols(f * width, width)].astype(F32)
    for copy in shards:
        copy.wait()
    for k in range(n - 1):
        total = total + p_in[k].astype(F32)
    s_own[...] = total.astype(BF16)
    swap = pltpu.make_async_remote_copy(
        src_ref=s_own, dst_ref=s_other, send_sem=s_send, recv_sem=s_recv,
        device_id={"rep": 1 - r}, device_id_type=MESH,
    )
    swap.start()
    kept = s_own[...].astype(F32)
    down_grad[pl.ds(pl.multiple_of(r * units, 16), units), :] = kept
    n_own[...] = lax.dot_general(
        jnp.ones((8, width), F32), kept * kept, (((1,), (1,)), ((), ())),
        precision=lax.Precision.HIGHEST, preferred_element_type=F32,
    )
    small = []
    for i, peer in enumerate(peers):
        copy = pltpu.make_async_remote_copy(
            src_ref=n_own, dst_ref=n_in.at[i], send_sem=n_send.at[i], recv_sem=n_recv.at[i],
            device_id=peer, device_id_type=MESH,
        )
        copy.start()
        small.append(copy)

    fourth.wait()
    fifth = push(4, g_out.at[:, cols(c * half, half)], g_out.at[:, cols(c * half, half)], {"tp": mate})
    for copy in small:
        copy.wait()
    here = n_own[...]
    for i in range(n - 1):
        here = here + n_in[i]
    there = n_in[n - 1]
    for i in range(n, 2 * n - 1):
        there = there + n_in[i]
    norms[pl.ds(r, 1)] = here[None]
    norms[pl.ds(1 - r, 1)] = there[None]
    swap.wait()
    down_grad[pl.ds(pl.multiple_of((1 - r) * units, 16), units), :] = s_other[...].astype(F32)
    fifth.wait()
    input_grad[...] = g_out[...]


def split_units(n, tokens, gate_weight, up_weight, down_weight, out_grad):
    rows, depth = tokens.shape
    width, both = gate_weight.shape
    units = both // 2
    start = lax.axis_index("rep") * units
    gate = lax.dynamic_slice_in_dim(gate_weight, start, units, 1).T
    up = lax.dynamic_slice_in_dim(up_weight, start, units, 1).T
    down = lax.dynamic_slice_in_dim(down_weight, start, units, 0)
    vmem = pl.BlockSpec(memory_space=pltpu.VMEM)
    anywhere = pl.BlockSpec(memory_space=pl.ANY)
    dma = pltpu.SemaphoreType.DMA
    whole = jax.ShapeDtypeStruct((units, depth), BF16)
    stacked = jax.ShapeDtypeStruct((2 * rows, depth), BF16)
    gate, up, down, tokens, grad = pl.pallas_call(
        functools.partial(gather_kernel, n),
        out_shape=[whole, whole, whole, stacked, stacked],
        in_specs=[vmem] * 5,
        out_specs=[anywhere] * 5,
        scratch_shapes=[dma((3, n - 1))] * 4 + [dma((2,)), dma((2,)), dma((5,))],
        compiler_params=pltpu.CompilerParams(collective_id=0, has_side_effects=True),
        name="gather",
    )(gate, up, down, tokens, out_grad)

    gate_pre = contract_last(tokens, gate)
    up_pre = contract_last(tokens, up)
    sigma = jax.nn.sigmoid(gate_pre)
    activated = gate_pre * sigma
    hidden = (activated * up_pre).astype(BF16)
    hid_grad = contract_last(grad, down)
    up_grad = (hid_grad * activated).astype(BF16)
    gate_grad = (hid_grad * up_pre * sigma * (1.0 + gate_pre * (1.0 - sigma))).astype(BF16)
    part = contract_first(hidden, grad).astype(BF16)
    flow = (
        jnp.dot(gate_grad, gate, preferred_element_type=F32)
        + jnp.dot(up_grad, up, preferred_element_type=F32)
    ).astype(BF16)

    half, quarter = depth // 2, depth // 4
    peers = 2 * n - 1
    input_grad, down_grad, norms = pl.pallas_call(
        functools.partial(reduce_kernel, n),
        out_shape=[
            jax.ShapeDtypeStruct((rows, depth), BF16),
            jax.ShapeDtypeStruct((both, width), F32),
            jax.ShapeDtypeStruct((2, 8, units), F32),
        ],
        in_specs=[vmem] * 2,
        out_specs=[vmem] * 3,
        scratch_shapes=[
            pltpu.VMEM((n - 1, units, width), BF16),
            pltpu.VMEM((2 * rows, half), BF16),
            pltpu.VMEM((2, rows, half), BF16),
            pltpu.VMEM((rows, half), BF16),
            pltpu.VMEM((2, rows, quarter), BF16),
            pltpu.VMEM((rows, quarter), BF16),
            pltpu.VMEM((rows, depth), BF16),
            pltpu.VMEM((units, width), BF16),
            pltpu.VMEM((units, width), BF16),
            pltpu.VMEM((8, units), F32),
            pltpu.VMEM((peers, 8, units), F32),
            dma((n - 1,)), dma((n - 1,)), dma((5,)), dma((5,)), dma, dma, dma((peers,)), dma((peers,)),
        ],
        compiler_params=pltpu.CompilerParams(collective_id=1, has_side_effects=True),
        name="reduce",
    )(part, flow)
    return input_grad, down_grad, norms[:, 0, :].reshape(both)


def whole_units(tokens, gate_weight, up_weight, down_weight, out_grad):
    down_full = lax.all_gather(down_weight, "fs", axis=1, tiled=True)
    gate_full = lax.all_gather(gate_weight, "fs", axis=0, tiled=True)
    up_full = lax.all_gather(up_weight, "fs", axis=0, tiled=True)
    gate_pre = jnp.dot(tokens, gate_full, preferred_element_type=F32)
    up_pre = jnp.dot(tokens, up_full, preferred_element_type=F32)
    sigma = jax.nn.sigmoid(gate_pre)
    activated = gate_pre * sigma
    hidden = (activated * up_pre).astype(BF16)
    hid_grad = contract_last(out_grad, down_full)
    up_grad = (hid_grad * activated).astype(BF16)
    gate_grad = (hid_grad * up_pre * sigma * (1.0 + gate_pre * (1.0 - sigma))).astype(BF16)
    partial_value = contract_last(gate_grad, gate_full) + contract_last(up_grad, up_full)
    input_grad = lax.psum(partial_value.astype(BF16), "tp")
    columns = lax.all_to_all(out_grad, "fs", split_axis=1, concat_axis=0, tiled=True)
    shard = contract_first(lax.all_gather(hidden, "fs", axis=0, tiled=True), columns)
    shard = lax.psum(shard.astype(BF16), "rep").astype(F32)
    norms = lax.psum(jnp.sum(shard * shard, axis=1), "fs")
    return (input_grad, shard, norms)


def solution(mesh):
    n, rep, tp = mesh.shape["fs"], mesh.shape["rep"], mesh.shape["tp"]

    def on_device(tokens, gate_weight, up_weight, down_weight, out_grad):
        width, both = gate_weight.shape
        if rep == 2 and tp == 4 and 2 <= n <= 4 and both % 32 == 0 and width % 128 == 0:
            return split_units(n, tokens, gate_weight, up_weight, down_weight, out_grad)
        return whole_units(tokens, gate_weight, up_weight, down_weight, out_grad)

    return jax.shard_map(
        on_device,
        mesh=mesh,
        in_specs=(
            P(("rep", "fs"), None),
            P("fs", "tp"),
            P("fs", "tp"),
            P("tp", "fs"),
            P(("rep", "fs"), None),
        ),
        out_specs=(P(("rep", "fs"), None), P("tp", "fs"), P("tp")),
        check_vma=False,
    )
```

```python
import functools

import jax
import jax.numpy as jnp
from jax import lax
from jax.experimental import pallas as pl
from jax.experimental.pallas import tpu as pltpu
from jax.sharding import PartitionSpec as P

MESH = pl.DeviceIdType.MESH
BF16 = jnp.bfloat16
F32 = jnp.float32


def contract_last(left, right):
    return lax.dot_general(left, right, (((1,), (1,)), ((), ())), preferred_element_type=F32)


def contract_first(left, right):
    return lax.dot_general(left, right, (((0,), (0,)), ((), ())), preferred_element_type=F32)


def block_kernel(
    n, gate, up, down, tokens, grad, input_grad, down_grad, norms,
    gate_all, up_all, down_all, tokens_all, grad_all,
    gate_pre, up_pre, gate_grad, up_grad, part, p_in, p_out,
    f_out, f_in, g_own, g_out, g_in, h_out, h_in, whole_out, s_own, s_other, n_own, n_in,
    w_send, w_recv, p_send, p_recv, pair_send, pair_recv, own_sem, g_send, g_recv,
    s_send, s_recv, n_send, n_recv,
):
    f = lax.axis_index("fs")
    r = lax.axis_index("rep")
    t = lax.axis_index("tp")
    c, x = lax.rem(t, 2), t // 2
    mate, far = {"tp": x * 2 + 1 - c}, {"tp": (1 - x) * 2 + c}
    pair = {"rep": 1 - r}
    rows, depth = tokens.shape
    units, width = gate.shape
    half, quarter = depth // 2, depth // 4

    barrier = pltpu.get_barrier_semaphore()
    peers = [{"rep": lax.rem(r + a, 2), "fs": lax.rem(f + k, n)}
             for a in range(2) for k in range(n) if a or k]
    for peer in peers + [mate, far]:
        pl.semaphore_signal(barrier, inc=1, device_id=peer, device_id_type=MESH)
    pl.semaphore_wait(barrier, 2 * n + 1)

    def cols(start, size):
        return pl.ds(pl.multiple_of(start, size), size)

    def remote(src, dst, send, recv, peer):
        return pltpu.make_async_remote_copy(
            src_ref=src, dst_ref=dst, send_sem=send, recv_sem=recv,
            device_id=peer, device_id_type=MESH,
        )

    shards = ((gate, gate_all), (up, up_all), (down, down_all))
    ways = (1, 0)

    def hop(w, step, way, arriving=False):
        own, whole = shards[w]
        sign = 1 if way else -1
        owner = f - sign * (step + 1 if arriving else step)
        place = whole.at[:, cols(owner * width, width)]
        return remote(
            own if step == 0 and not arriving else place, place,
            w_send.at[way, w, step], w_recv.at[way, w, step],
            {"fs": f - sign if arriving else f + sign},
        )

    def sends(step, way):
        return (f < n - 1) & (f >= step) if way else (f > 0) & (f + step <= n - 1)

    def receives(step, way):
        return f - 1 - step >= 0 if way else f + 1 + step <= n - 1

    def forward(w, step):
        for way in ways:
            @pl.when(sends(step, way))
            def _():
                hop(w, step, way).start()

    def arrive(w, step):
        for way in ways:
            @pl.when(receives(step, way))
            def _():
                hop(w, step, way, True).wait_recv()

    for w in range(2):
        forward(w, 0)
    pairs = []
    for i, (own, whole) in enumerate(((tokens, tokens_all), (grad, grad_all))):
        copy = remote(own, whole.at[pl.ds(rows, rows)], pair_send.at[i], pair_recv.at[i], pair)
        copy.start()
        pairs.append(copy)
    local = []
    for i, (own, place) in enumerate((
        (tokens, tokens_all.at[pl.ds(0, rows)]),
        (grad, grad_all.at[pl.ds(0, rows)]),
        (gate, gate_all.at[:, cols(f * width, width)]),
        (up, up_all.at[:, cols(f * width, width)]),
        (down, down_all.at[:, cols(f * width, width)]),
    )):
        copy = pltpu.make_async_copy(own, place, own_sem.at[i])
        copy.start()
        local.append(copy)

    for step in range(n - 1):
        if step == n - 2:
            forward(2, 0)
        for w in range(2):
            arrive(w, step)
            if step + 1 < n - 1:
                forward(w, step + 1)
    for copy in pairs + local:
        copy.wait()

    for b in range(2):
        span = pl.ds(b * rows, rows)
        gate_pre[span] = contract_last(tokens_all[span], gate_all[...])
        up_pre[span] = contract_last(tokens_all[span], up_all[...])

    def relay_down(step):
        arrive(2, step)
        if step + 1 < n - 1:
            forward(2, step + 1)

    relay_down(0)
    pre = gate_pre[...]
    hidden = (pre * jax.nn.sigmoid(pre) * up_pre[...]).astype(BF16)
    for k in range(n):
        at = pl.ds(k * width, width)
        part[:, at] = contract_first(hidden, grad_all[:, at]).astype(BF16)

    def sum_goes(step, way):
        return f <= n - 2 - step if way else f >= step + 1

    def sum_comes(step, way):
        return (f >= 1) & (f <= n - 1 - step) if way else (f <= n - 2) & (f >= step)

    def sum_copy(step, way, first):
        target = n - 1 - step if way else step
        return remote(
            part.at[:, pl.ds(target * width, width)] if first else p_out.at[way, step],
            p_in.at[way, step], p_send.at[way, step], p_recv.at[way, step],
            {"fs": f + 1 if way else f - 1},
        )

    def at_end(way):
        return f == 0 if way else f == n - 1

    for step in range(n - 1):
        for way in ways:
            @pl.when(at_end(way))
            def _():
                sum_copy(step, way, True).start()

    def relay_sum(step):
        for way in ways:
            target = n - 1 - step if way else step

            @pl.when(sum_comes(step, way))
            def _():
                sum_copy(step, way, False).wait_recv()

            @pl.when(sum_comes(step, way) & sum_goes(step, way))
            def _():
                p_out[way, step] = (
                    part[:, pl.ds(target * width, width)].astype(F32) + p_in[way, step].astype(F32)
                ).astype(BF16)
                sum_copy(step, way, False).start()

    for step in range(1, n - 1):
        relay_down(step)

    for b in range(2):
        span = pl.ds(b * rows, rows)
        hid = contract_last(grad_all[span], down_all[...])
        pre = gate_pre[span]
        sigma = jax.nn.sigmoid(pre)
        up_grad[span] = (hid * (pre * sigma)).astype(BF16)
        gate_grad[span] = (hid * up_pre[span] * sigma * (1.0 + pre * (1.0 - sigma))).astype(BF16)

    def flow(b, at):
        span = pl.ds(b * rows, rows)
        return (
            jnp.dot(gate_grad[span], gate_all[:, at], preferred_element_type=F32)
            + jnp.dot(up_grad[span], up_all[:, at], preferred_element_type=F32)
        )

    def push(i, src, dst, peer):
        copy = remote(src, dst, g_send.at[i], g_recv.at[i], peer)
        copy.start()
        return copy

    cross = {}
    for b in (1, 0):
        f_out[b] = flow(b, cols((1 - c) * half, half)).astype(BF16)
        cross[b] = push(b, f_out.at[b], f_in.at[b], mate)
    for b in (1, 0):
        kept = flow(b, cols(c * half, half))
        cross[b].wait()
        kept = kept + f_in[b].astype(F32)
        for q in range(2):
            piece = kept[:, q * quarter:(q + 1) * quarter]
            if b == 1:
                g_out[q] = piece.astype(BF16)
            else:
                g_own[q] = piece
        if b == 1:
            early = push(2, g_out.at[1 - x], g_in.at[1 - x], pair)
            late = push(3, g_out.at[x], g_in.at[x], pair)
    relay_sum(0)
    early.wait()
    h_out[...] = (g_own[1 - x] + g_in[1 - x].astype(F32)).astype(BF16)
    over = push(4, h_out, h_in, far)
    for step in range(1, n - 1):
        relay_sum(step)

    def finish(way):
        step = n - 1 - f if way else f
        return p_in[way, lax.rem(step, n - 1)].astype(F32)

    s_sum = part[:, cols(f * width, width)].astype(F32)
    s_sum = s_sum + jnp.where(f > 0, finish(1), 0.0) + jnp.where(f < n - 1, finish(0), 0.0)
    s_own[...] = s_sum.astype(BF16)
    late.wait()
    over.wait()
    mine = cols(c * half + x * quarter, quarter)
    theirs = cols(c * half + (1 - x) * quarter, quarter)
    whole_out[:, mine] = (
        g_own[x] + g_in[x].astype(F32) + h_in[...].astype(F32)
    ).astype(BF16)
    across = push(5, whole_out.at[:, mine], whole_out.at[:, mine], far)
    beside = push(6, whole_out.at[:, mine], whole_out.at[:, mine], mate)
    swap = remote(s_own, s_other, s_send, s_recv, pair)
    swap.start()

    kept = s_own[...].astype(F32)
    down_grad[pl.ds(pl.multiple_of(r * units, 16), units), :] = kept
    n_own[...] = lax.dot_general(
        jnp.ones((8, width), F32), kept * kept, (((1,), (1,)), ((), ())),
        precision=lax.Precision.HIGHEST, preferred_element_type=F32,
    )
    small = []
    for i, peer in enumerate(peers):
        copy = remote(n_own, n_in.at[i], n_send.at[i], n_recv.at[i], peer)
        copy.start()
        small.append(copy)
    for step in range(n - 1):
        for way in ways:
            for w in range(3):
                @pl.when(sends(step, way))
                def _():
                    hop(w, step, way).wait_send()

            @pl.when(sum_goes(step, way))
            def _():
                sum_copy(step, way, False).wait_send()
    swap.wait()
    down_grad[pl.ds(pl.multiple_of((1 - r) * units, 16), units), :] = s_other[...].astype(F32)
    across.wait()
    last = push(7, whole_out.at[:, theirs], whole_out.at[:, theirs], mate)
    for copy in small:
        copy.wait()
    here = n_own[...]
    for i in range(n - 1):
        here = here + n_in[i]
    there = n_in[n - 1]
    for i in range(n, 2 * n - 1):
        there = there + n_in[i]
    norms[pl.ds(r, 1)] = here[None]
    norms[pl.ds(1 - r, 1)] = there[None]
    beside.wait()
    last.wait()
    input_grad[...] = whole_out[...]


def split_units(n, tokens, gate_weight, up_weight, down_weight, out_grad):
    rows, depth = tokens.shape
    width, both = gate_weight.shape
    units = both // 2
    start = lax.axis_index("rep") * units
    gate = lax.dynamic_slice_in_dim(gate_weight, start, units, 1).T
    up = lax.dynamic_slice_in_dim(up_weight, start, units, 1).T
    down = lax.dynamic_slice_in_dim(down_weight, start, units, 0)
    vmem = pl.BlockSpec(memory_space=pltpu.VMEM)
    dma = pltpu.SemaphoreType.DMA
    half, quarter = depth // 2, depth // 4
    peers = 2 * n - 1
    scratch = [((units, depth), BF16)] * 3 + [((2 * rows, depth), BF16)] * 2
    scratch += [((2 * rows, units), F32)] * 2 + [((2 * rows, units), BF16)] * 2
    scratch += [((units, depth), BF16)] + [((2, n - 1, units, width), BF16)] * 2
    scratch += [((2, rows, half), BF16)] * 2 + [((2, rows, quarter), F32)]
    scratch += [((2, rows, quarter), BF16)] * 2 + [((rows, quarter), BF16)] * 2
    scratch += [((rows, depth), BF16)] + [((units, width), BF16)] * 2
    scratch += [((8, units), F32), ((peers, 8, units), F32)]
    input_grad, down_grad, norms = pl.pallas_call(
        functools.partial(block_kernel, n),
        out_shape=[
            jax.ShapeDtypeStruct((rows, depth), BF16),
            jax.ShapeDtypeStruct((both, width), F32),
            jax.ShapeDtypeStruct((2, 8, units), F32),
        ],
        in_specs=[vmem] * 5,
        out_specs=[vmem] * 3,
        scratch_shapes=[pltpu.VMEM(shape, kind) for shape, kind in scratch] + [
            dma((2, 3, n - 1)), dma((2, 3, n - 1)), dma((2, n - 1)), dma((2, n - 1)),
            dma((2,)), dma((2,)), dma((5,)), dma((8,)), dma((8,)),
            dma, dma, dma((peers,)), dma((peers,)),
        ],
        compiler_params=pltpu.CompilerParams(collective_id=0, has_side_effects=True),
        name="block",
    )(gate, up, down, tokens, out_grad)
    return input_grad, down_grad, norms[:, 0, :].reshape(both)


def whole_units(tokens, gate_weight, up_weight, down_weight, out_grad):
    down_full = lax.all_gather(down_weight, "fs", axis=1, tiled=True)
    gate_full = lax.all_gather(gate_weight, "fs", axis=0, tiled=True)
    up_full = lax.all_gather(up_weight, "fs", axis=0, tiled=True)
    gate_pre = jnp.dot(tokens, gate_full, preferred_element_type=F32)
    up_pre = jnp.dot(tokens, up_full, preferred_element_type=F32)
    sigma = jax.nn.sigmoid(gate_pre)
    activated = gate_pre * sigma
    hidden = (activated * up_pre).astype(BF16)
    hid_grad = contract_last(out_grad, down_full)
    up_grad = (hid_grad * activated).astype(BF16)
    gate_grad = (hid_grad * up_pre * sigma * (1.0 + gate_pre * (1.0 - sigma))).astype(BF16)
    partial_value = contract_last(gate_grad, gate_full) + contract_last(up_grad, up_full)
    input_grad = lax.psum(partial_value.astype(BF16), "tp")
    columns = lax.all_to_all(out_grad, "fs", split_axis=1, concat_axis=0, tiled=True)
    shard = contract_first(lax.all_gather(hidden, "fs", axis=0, tiled=True), columns)
    shard = lax.psum(shard.astype(BF16), "rep").astype(F32)
    norms = lax.psum(jnp.sum(shard * shard, axis=1), "fs")
    return (input_grad, shard, norms)


def solution(mesh):
    n, rep, tp = mesh.shape["fs"], mesh.shape["rep"], mesh.shape["tp"]

    def on_device(tokens, gate_weight, up_weight, down_weight, out_grad):
        width, both = gate_weight.shape
        if rep == 2 and tp == 4 and 2 <= n <= 4 and both % 32 == 0 and width % 128 == 0:
            return split_units(n, tokens, gate_weight, up_weight, down_weight, out_grad)
        return whole_units(tokens, gate_weight, up_weight, down_weight, out_grad)

    return jax.shard_map(
        on_device,
        mesh=mesh,
        in_specs=(
            P(("rep", "fs"), None),
            P("fs", "tp"),
            P("fs", "tp"),
            P("tp", "fs"),
            P(("rep", "fs"), None),
        ),
        out_specs=(P(("rep", "fs"), None), P("tp", "fs"), P("tp")),
        check_vma=False,
    )
```

```python
import functools

import jax
import jax.numpy as jnp
from jax import lax
from jax.experimental import pallas as pl
from jax.experimental.pallas import tpu as pltpu
from jax.sharding import PartitionSpec as P

MESH = pl.DeviceIdType.MESH
BF16 = jnp.bfloat16
F32 = jnp.float32


def contract_last(left, right):
    return lax.dot_general(left, right, (((1,), (1,)), ((), ())), preferred_element_type=F32)


def contract_first(left, right):
    return lax.dot_general(left, right, (((0,), (0,)), ((), ())), preferred_element_type=F32)


def block_kernel(
    n, gate, up, down, tokens, grad, input_grad, down_grad, norms,
    gate_all, up_all, down_all, tokens_all, grad_all,
    gate_pre, up_pre, gate_grad, up_grad, part, p_in, p_out,
    f_out, f_in, g_own, g_out, g_in, h_out, h_in, whole_out, s_own, s_other, n_own, n_in,
    w_send, w_recv, p_send, p_recv, pair_send, pair_recv, own_sem, g_send, g_recv,
    s_send, s_recv, n_send, n_recv,
):
    f = lax.axis_index("fs")
    r = lax.axis_index("rep")
    t = lax.axis_index("tp")
    c, x = lax.rem(t, 2), t // 2
    mate, far = {"tp": x * 2 + 1 - c}, {"tp": (1 - x) * 2 + c}
    pair = {"rep": 1 - r}
    rows, depth = tokens.shape
    units, width = gate.shape
    half = depth // 2
    pieces = g_out.shape[0]
    size = half // pieces
    down_half = down.at[pl.ds(pl.multiple_of(r * units, 16), units)]

    barrier = pltpu.get_barrier_semaphore()
    peers = [{"rep": lax.rem(r + a, 2), "fs": lax.rem(f + k, n)}
             for a in range(2) for k in range(n) if a or k]
    for peer in peers + [mate, far]:
        pl.semaphore_signal(barrier, inc=1, device_id=peer, device_id_type=MESH)
    pl.semaphore_wait(barrier, 2 * n + 1)

    def cols(start, size):
        return pl.ds(pl.multiple_of(start, size), size)

    def remote(src, dst, send, recv, peer):
        return pltpu.make_async_remote_copy(
            src_ref=src, dst_ref=dst, send_sem=send, recv_sem=recv,
            device_id=peer, device_id_type=MESH,
        )

    shards = ((gate, gate_all), (up, up_all), (down_half, down_all))
    ways = (1, 0)

    def hop(w, step, way, arriving=False):
        own, whole = shards[w]
        sign = 1 if way else -1
        owner = f - sign * (step + 1 if arriving else step)
        place = whole.at[:, cols(owner * width, width)]
        return remote(
            own if step == 0 and not arriving else place, place,
            w_send.at[way, w, step], w_recv.at[way, w, step],
            {"fs": f - sign if arriving else f + sign},
        )

    def sends(step, way):
        return (f < n - 1) & (f >= step) if way else (f > 0) & (f + step <= n - 1)

    def receives(step, way):
        return f - 1 - step >= 0 if way else f + 1 + step <= n - 1

    def forward(w, step):
        for way in ways:
            @pl.when(sends(step, way))
            def _():
                hop(w, step, way).start()

    def arrive(w, step):
        for way in ways:
            @pl.when(receives(step, way))
            def _():
                hop(w, step, way, True).wait_recv()

    for w in range(2):
        forward(w, 0)
    pairs = []
    for i, (own, whole) in enumerate(((tokens, tokens_all), (grad, grad_all))):
        copy = remote(own, whole.at[pl.ds(rows, rows)], pair_send.at[i], pair_recv.at[i], pair)
        copy.start()
        pairs.append(copy)
    local = []
    for i, (own, place) in enumerate((
        (tokens, tokens_all.at[pl.ds(0, rows)]),
        (grad, grad_all.at[pl.ds(0, rows)]),
        (gate, gate_all.at[:, cols(f * width, width)]),
        (up, up_all.at[:, cols(f * width, width)]),
        (down_half, down_all.at[:, cols(f * width, width)]),
    )):
        copy = pltpu.make_async_copy(own, place, own_sem.at[i])
        copy.start()
        local.append(copy)

    for step in range(n - 1):
        if step == n - 2:
            forward(2, 0)
        for w in range(2):
            arrive(w, step)
            if step + 1 < n - 1:
                forward(w, step + 1)
    for copy in pairs + local:
        copy.wait()

    for b in range(2):
        span = pl.ds(b * rows, rows)
        gate_pre[span] = contract_last(tokens_all[span], gate_all[...])
        up_pre[span] = contract_last(tokens_all[span], up_all[...])

    def relay_down(step):
        arrive(2, step)
        if step + 1 < n - 1:
            forward(2, step + 1)

    relay_down(0)
    pre = gate_pre[...]
    hidden = (pre * jax.nn.sigmoid(pre) * up_pre[...]).astype(BF16)
    for k in range(n):
        at = pl.ds(k * width, width)
        part[:, at] = contract_first(hidden, grad_all[:, at]).astype(BF16)

    def sum_goes(step, way):
        return f <= n - 2 - step if way else f >= step + 1

    def sum_comes(step, way):
        return (f >= 1) & (f <= n - 1 - step) if way else (f <= n - 2) & (f >= step)

    def sum_copy(step, way, first):
        target = n - 1 - step if way else step
        return remote(
            part.at[:, pl.ds(target * width, width)] if first else p_out.at[way, step],
            p_in.at[way, step], p_send.at[way, step], p_recv.at[way, step],
            {"fs": f + 1 if way else f - 1},
        )

    def at_end(way):
        return f == 0 if way else f == n - 1

    for step in range(n - 1):
        for way in ways:
            @pl.when(at_end(way))
            def _():
                sum_copy(step, way, True).start()

    def relay_sum(step, hops):
        for way in ways:
            target = n - 1 - step if way else step
            here = f == hops if way else f == n - 1 - hops

            @pl.when(sum_comes(step, way) & here)
            def _():
                sum_copy(step, way, False).wait_recv()

            @pl.when(sum_comes(step, way) & sum_goes(step, way) & here)
            def _():
                p_out[way, step] = (
                    part[:, pl.ds(target * width, width)].astype(F32) + p_in[way, step].astype(F32)
                ).astype(BF16)
                sum_copy(step, way, False).start()

    def relay_sums(when):
        for step in range(n - 1):
            hops = when - step
            if 1 <= hops <= n - 1 - step:
                relay_sum(step, hops)

    for step in range(1, n - 1):
        relay_down(step)
        if step == 1:
            relay_sums(1)
    if n == 2:
        relay_sums(1)

    for b in range(2):
        span = pl.ds(b * rows, rows)
        hid = contract_last(grad_all[span], down_all[...])
        pre = gate_pre[span]
        sigma = jax.nn.sigmoid(pre)
        up_grad[span] = (hid * (pre * sigma)).astype(BF16)
        gate_grad[span] = (hid * up_pre[span] * sigma * (1.0 + pre * (1.0 - sigma))).astype(BF16)

    def flow(b, at):
        span = pl.ds(b * rows, rows)
        return (
            jnp.dot(gate_grad[span], gate_all[:, at], preferred_element_type=F32)
            + jnp.dot(up_grad[span], up_all[:, at], preferred_element_type=F32)
        )

    def push(i, src, dst, peer):
        copy = remote(src, dst, g_send.at[i], g_recv.at[i], peer)
        copy.start()
        return copy

    cross = {}
    for b in (1, 0):
        f_out[b] = flow(b, cols((1 - c) * half, half)).astype(BF16)
        cross[b] = push(b, f_out.at[b], f_in.at[b], mate)
    over = []
    for b in (1, 0):
        kept = flow(b, cols(c * half, half))
        cross[b].wait()
        kept = kept + f_in[b].astype(F32)
        for q in range(pieces):
            piece = kept[:, q * size:(q + 1) * size]
            if b == 1:
                g_out[q] = piece.astype(BF16)
                over.append(push(2 + q, g_out.at[q], g_in.at[q], pair))
            else:
                g_own[q] = piece
    relay_sums(2)
    across = []
    for q in range(pieces):
        over[q].wait()
        h_out[q] = (g_own[q] + g_in[q].astype(F32)).astype(BF16)
        across.append(push(2 + pieces + q, h_out.at[q], h_in.at[q], far))
    for when in range(3, n):
        relay_sums(when)

    def finish(way):
        step = n - 1 - f if way else f
        return p_in[way, lax.rem(step, n - 1)].astype(F32)

    s_sum = part[:, cols(f * width, width)].astype(F32)
    s_sum = s_sum + jnp.where(f > 0, finish(1), 0.0) + jnp.where(f < n - 1, finish(0), 0.0)
    s_own[...] = s_sum.astype(BF16)
    swap = remote(s_own, s_other, s_send, s_recv, pair)
    swap.start()

    kept = s_own[...].astype(F32)
    down_grad[pl.ds(pl.multiple_of(r * units, 16), units), :] = s_own[...]
    n_own[...] = lax.dot_general(
        jnp.ones((8, width), F32), kept * kept, (((1,), (1,)), ((), ())),
        precision=lax.Precision.HIGHEST, preferred_element_type=F32,
    )
    small = []
    for i, peer in enumerate(peers):
        copy = remote(n_own, n_in.at[i], n_send.at[i], n_recv.at[i], peer)
        copy.start()
        small.append(copy)
    beside = []
    for q in range(pieces):
        across[q].wait()
        at = cols(c * half + q * size, size)
        whole_out[:, at] = (h_out[q].astype(F32) + h_in[q].astype(F32)).astype(BF16)
        beside.append(push(2 + 2 * pieces + q, whole_out.at[:, at], whole_out.at[:, at], mate))
    for step in range(n - 1):
        for way in ways:
            for w in range(3):
                @pl.when(sends(step, way))
                def _():
                    hop(w, step, way).wait_send()

            @pl.when(sum_goes(step, way))
            def _():
                sum_copy(step, way, False).wait_send()
    for copy in small:
        copy.wait()
    here = n_own[...]
    for i in range(n - 1):
        here = here + n_in[i]
    there = n_in[n - 1]
    for i in range(n, 2 * n - 1):
        there = there + n_in[i]
    norms[...] = jnp.concatenate(
        [jnp.where(r == 0, here, there), jnp.where(r == 0, there, here)], axis=1
    )
    swap.wait()
    down_grad[pl.ds(pl.multiple_of((1 - r) * units, 16), units), :] = s_other[...]
    for copy in beside:
        copy.wait()
    input_grad[...] = whole_out[...]


def split_units(n, tokens, gate_weight, up_weight, down_weight, out_grad):
    rows, depth = tokens.shape
    width, both = gate_weight.shape
    units = both // 2
    start = lax.axis_index("rep") * units
    gate = lax.dynamic_slice_in_dim(gate_weight, start, units, 1).T
    up = lax.dynamic_slice_in_dim(up_weight, start, units, 1).T
    anywhere = pl.BlockSpec(memory_space=pl.ANY)
    vmem = pl.BlockSpec(memory_space=pltpu.VMEM)
    dma = pltpu.SemaphoreType.DMA
    half, pieces = depth // 2, 4
    piece = (pieces, rows, half // pieces)
    peers = 2 * n - 1
    scratch = [((units, depth), BF16)] * 3 + [((2 * rows, depth), BF16)] * 2
    scratch += [((2 * rows, units), F32)] * 2 + [((2 * rows, units), BF16)] * 2
    scratch += [((units, depth), BF16)] + [((2, n - 1, units, width), BF16)] * 2
    scratch += [((2, rows, half), BF16)] * 2 + [(piece, F32)] + [(piece, BF16)] * 4
    scratch += [((rows, depth), BF16)] + [((units, width), BF16)] * 2
    scratch += [((8, units), F32), ((peers, 8, units), F32)]
    input_grad, down_grad, norms = pl.pallas_call(
        functools.partial(block_kernel, n),
        out_shape=[
            jax.ShapeDtypeStruct((rows, depth), BF16),
            jax.ShapeDtypeStruct((both, width), BF16),
            jax.ShapeDtypeStruct((8, both), F32),
        ],
        in_specs=[vmem] * 2 + [anywhere] * 3,
        out_specs=[vmem] * 3,
        scratch_shapes=[pltpu.VMEM(shape, kind) for shape, kind in scratch] + [
            dma((2, 3, n - 1)), dma((2, 3, n - 1)), dma((2, n - 1)), dma((2, n - 1)),
            dma((2,)), dma((2,)), dma((5,)), dma((2 + 3 * pieces,)), dma((2 + 3 * pieces,)),
            dma, dma, dma((peers,)), dma((peers,)),
        ],
        compiler_params=pltpu.CompilerParams(collective_id=0, has_side_effects=True),
        name="block",
    )(gate, up, down_weight, tokens, out_grad)
    return input_grad, down_grad.astype(F32), norms[0]


def whole_units(tokens, gate_weight, up_weight, down_weight, out_grad):
    down_full = lax.all_gather(down_weight, "fs", axis=1, tiled=True)
    gate_full = lax.all_gather(gate_weight, "fs", axis=0, tiled=True)
    up_full = lax.all_gather(up_weight, "fs", axis=0, tiled=True)
    gate_pre = jnp.dot(tokens, gate_full, preferred_element_type=F32)
    up_pre = jnp.dot(tokens, up_full, preferred_element_type=F32)
    sigma = jax.nn.sigmoid(gate_pre)
    activated = gate_pre * sigma
    hidden = (activated * up_pre).astype(BF16)
    hid_grad = contract_last(out_grad, down_full)
    up_grad = (hid_grad * activated).astype(BF16)
    gate_grad = (hid_grad * up_pre * sigma * (1.0 + gate_pre * (1.0 - sigma))).astype(BF16)
    partial_value = contract_last(gate_grad, gate_full) + contract_last(up_grad, up_full)
    input_grad = lax.psum(partial_value.astype(BF16), "tp")
    columns = lax.all_to_all(out_grad, "fs", split_axis=1, concat_axis=0, tiled=True)
    shard = contract_first(lax.all_gather(hidden, "fs", axis=0, tiled=True), columns)
    shard = lax.psum(shard.astype(BF16), "rep").astype(F32)
    norms = lax.psum(jnp.sum(shard * shard, axis=1), "fs")
    return (input_grad, shard, norms)


def solution(mesh):
    n, rep, tp = mesh.shape["fs"], mesh.shape["rep"], mesh.shape["tp"]

    def on_device(tokens, gate_weight, up_weight, down_weight, out_grad):
        width, both = gate_weight.shape
        if rep == 2 and tp == 4 and 2 <= n <= 4 and both % 32 == 0 and width % 128 == 0:
            return split_units(n, tokens, gate_weight, up_weight, down_weight, out_grad)
        return whole_units(tokens, gate_weight, up_weight, down_weight, out_grad)

    return jax.shard_map(
        on_device,
        mesh=mesh,
        in_specs=(
            P(("rep", "fs"), None),
            P("fs", "tp"),
            P("fs", "tp"),
            P("tp", "fs"),
            P(("rep", "fs"), None),
        ),
        out_specs=(P(("rep", "fs"), None), P("tp", "fs"), P("tp")),
        check_vma=False,
    )
```

```python
import functools

import jax
import jax.numpy as jnp
from jax import lax
from jax.experimental import pallas as pl
from jax.experimental.pallas import tpu as pltpu
from jax.sharding import PartitionSpec as P

MESH = pl.DeviceIdType.MESH
BF16 = jnp.bfloat16
F32 = jnp.float32


def contract_last(left, right):
    return lax.dot_general(left, right, (((1,), (1,)), ((), ())), preferred_element_type=F32)


def contract_first(left, right):
    return lax.dot_general(left, right, (((0,), (0,)), ((), ())), preferred_element_type=F32)


def block_kernel(
    n, gate, up, down, tokens, grad, input_grad, down_grad, norms,
    gate_all, up_all, down_all, tokens_all, grad_all,
    gate_pre, up_pre, hid, gate_grad, up_grad, part, p_in, p_out,
    f_out, f_in, g_own, g_out, g_in, h_out, h_in, whole_out, s_own, s_other, n_own, n_in,
    w_send, w_recv, p_send, p_recv, pair_send, pair_recv, own_sem, g_send, g_recv,
    s_send, s_recv, n_send, n_recv,
):
    f = lax.axis_index("fs")
    r = lax.axis_index("rep")
    t = lax.axis_index("tp")
    c, x = lax.rem(t, 2), t // 2
    mate, far = {"tp": x * 2 + 1 - c}, {"tp": (1 - x) * 2 + c}
    pair = {"rep": 1 - r}
    rows, depth = tokens.shape
    units, width = gate.shape
    half = depth // 2
    pieces = g_out.shape[0]
    size = half // pieces
    down_half = down.at[pl.ds(pl.multiple_of(r * units, 16), units)]

    barrier = pltpu.get_barrier_semaphore()
    peers = [{"rep": lax.rem(r + a, 2), "fs": lax.rem(f + k, n)}
             for a in range(2) for k in range(n) if a or k]
    for peer in peers + [mate, far]:
        pl.semaphore_signal(barrier, inc=1, device_id=peer, device_id_type=MESH)
    pl.semaphore_wait(barrier, 2 * n + 1)

    def cols(start, size):
        return pl.ds(pl.multiple_of(start, size), size)

    def remote(src, dst, send, recv, peer):
        return pltpu.make_async_remote_copy(
            src_ref=src, dst_ref=dst, send_sem=send, recv_sem=recv,
            device_id=peer, device_id_type=MESH,
        )

    shards = ((gate, gate_all), (up, up_all), (down_half, down_all))
    ways = (1, 0)

    def hop(w, step, way, arriving=False):
        own, whole = shards[w]
        sign = 1 if way else -1
        owner = f - sign * (step + 1 if arriving else step)
        place = whole.at[:, cols(owner * width, width)]
        return remote(
            own if step == 0 and not arriving else place, place,
            w_send.at[way, w, step], w_recv.at[way, w, step],
            {"fs": f - sign if arriving else f + sign},
        )

    def sends(step, way):
        return (f < n - 1) & (f >= step) if way else (f > 0) & (f + step <= n - 1)

    def receives(step, way):
        return f - 1 - step >= 0 if way else f + 1 + step <= n - 1

    def forward(w, step):
        for way in ways:
            @pl.when(sends(step, way))
            def _():
                hop(w, step, way).start()

    def arrive(w, step):
        for way in ways:
            @pl.when(receives(step, way))
            def _():
                hop(w, step, way, True).wait_recv()

    for w in range(2):
        forward(w, 0)
    pairs = []
    for i, (own, whole) in enumerate(((tokens, tokens_all), (grad, grad_all))):
        copy = remote(own, whole.at[pl.ds(rows, rows)], pair_send.at[i], pair_recv.at[i], pair)
        copy.start()
        pairs.append(copy)
    local = []
    for i, (own, place) in enumerate((
        (tokens, tokens_all.at[pl.ds(0, rows)]),
        (grad, grad_all.at[pl.ds(0, rows)]),
        (gate, gate_all.at[:, cols(f * width, width)]),
        (up, up_all.at[:, cols(f * width, width)]),
        (down_half, down_all.at[:, cols(f * width, width)]),
    )):
        copy = pltpu.make_async_copy(own, place, own_sem.at[i])
        copy.start()
        local.append(copy)

    for step in range(n - 1):
        if step == n - 2:
            forward(2, 0)
        for w in range(2):
            arrive(w, step)
            if step + 1 < n - 1:
                forward(w, step + 1)
    for copy in pairs + local:
        copy.wait()

    for b in range(2):
        span = pl.ds(b * rows, rows)
        gate_pre[span] = contract_last(tokens_all[span], gate_all[...])
        up_pre[span] = contract_last(tokens_all[span], up_all[...])

    def relay_down(step):
        arrive(2, step)
        if step + 1 < n - 1:
            forward(2, step + 1)

    relay_down(0)
    pre, raw = gate_pre[...], up_pre[...]
    sigma = jax.nn.sigmoid(pre)
    hidden = (pre * sigma * raw).astype(BF16)
    gate_pre[...] = pre * sigma
    up_pre[...] = raw * sigma * (1.0 + pre * (1.0 - sigma))
    for k in range(n):
        at = pl.ds(k * width, width)
        part[:, at] = contract_first(hidden, grad_all[:, at]).astype(BF16)

    def sum_goes(step, way):
        return f <= n - 2 - step if way else f >= step + 1

    def sum_comes(step, way):
        return (f >= 1) & (f <= n - 1 - step) if way else (f <= n - 2) & (f >= step)

    def sum_copy(step, way, first):
        target = n - 1 - step if way else step
        return remote(
            part.at[:, pl.ds(target * width, width)] if first else p_out.at[way, step],
            p_in.at[way, step], p_send.at[way, step], p_recv.at[way, step],
            {"fs": f + 1 if way else f - 1},
        )

    def at_end(way):
        return f == 0 if way else f == n - 1

    for step in range(n - 1):
        for way in ways:
            @pl.when(at_end(way))
            def _():
                sum_copy(step, way, True).start()

    def relay_sum(step, hops):
        for way in ways:
            target = n - 1 - step if way else step
            here = f == hops if way else f == n - 1 - hops

            @pl.when(sum_comes(step, way) & here)
            def _():
                sum_copy(step, way, False).wait_recv()

            @pl.when(sum_comes(step, way) & sum_goes(step, way) & here)
            def _():
                p_out[way, step] = (
                    part[:, pl.ds(target * width, width)].astype(F32) + p_in[way, step].astype(F32)
                ).astype(BF16)
                sum_copy(step, way, False).start()

    def relay_sums(when):
        for step in range(n - 1):
            hops = when - step
            if 1 <= hops <= n - 1 - step:
                relay_sum(step, hops)

    def add_shard(owner):
        at = cols(owner * width, width)
        hid[...] += contract_last(grad_all[:, at], down_all[:, at])

    def add_shards(step):
        for way in ways:
            @pl.when(receives(step, way))
            def _():
                add_shard(f - 1 - step if way else f + 1 + step)

    mine = cols(f * width, width)
    hid[...] = contract_last(grad_all[:, mine], down_all[:, mine])
    add_shards(0)
    for step in range(1, n - 1):
        relay_down(step)
        add_shards(step)
        if step == 1:
            relay_sums(1)
    if n == 2:
        relay_sums(1)

    for b in range(2):
        span = pl.ds(b * rows, rows)
        up_grad[span] = (hid[span] * gate_pre[span]).astype(BF16)
        gate_grad[span] = (hid[span] * up_pre[span]).astype(BF16)

    def flow(b, at):
        span = pl.ds(b * rows, rows)
        return (
            jnp.dot(gate_grad[span], gate_all[:, at], preferred_element_type=F32)
            + jnp.dot(up_grad[span], up_all[:, at], preferred_element_type=F32)
        )

    def push(i, src, dst, peer):
        copy = remote(src, dst, g_send.at[i], g_recv.at[i], peer)
        copy.start()
        return copy

    cross = {}
    for b in (1, 0):
        f_out[b] = flow(b, cols((1 - c) * half, half)).astype(BF16)
        cross[b] = push(b, f_out.at[b], f_in.at[b], mate)
    over = []
    for b in (1, 0):
        kept = flow(b, cols(c * half, half))
        cross[b].wait()
        kept = kept + f_in[b].astype(F32)
        for q in range(pieces):
            piece = kept[:, q * size:(q + 1) * size]
            if b == 1:
                g_out[q] = piece.astype(BF16)
                over.append(push(2 + q, g_out.at[q], g_in.at[q], pair))
            else:
                g_own[q] = piece
    relay_sums(2)
    across = []
    for q in range(pieces):
        over[q].wait()
        h_out[q] = (g_own[q] + g_in[q].astype(F32)).astype(BF16)
        across.append(push(2 + pieces + q, h_out.at[q], h_in.at[q], far))
    for when in range(3, n):
        relay_sums(when)

    def finish(way):
        step = n - 1 - f if way else f
        return p_in[way, lax.rem(step, n - 1)].astype(F32)

    s_sum = part[:, cols(f * width, width)].astype(F32)
    s_sum = s_sum + jnp.where(f > 0, finish(1), 0.0) + jnp.where(f < n - 1, finish(0), 0.0)
    s_own[...] = s_sum.astype(BF16)
    swap = remote(s_own, s_other, s_send, s_recv, pair)
    swap.start()

    kept = s_own[...].astype(F32)
    down_grad[pl.ds(pl.multiple_of(r * units, 16), units), :] = s_own[...]
    n_own[...] = lax.dot_general(
        jnp.ones((8, width), F32), kept * kept, (((1,), (1,)), ((), ())),
        precision=lax.Precision.HIGHEST, preferred_element_type=F32,
    )
    small = []
    for i, peer in enumerate(peers):
        copy = remote(n_own, n_in.at[i], n_send.at[i], n_recv.at[i], peer)
        copy.start()
        small.append(copy)
    beside = []
    for q in range(pieces):
        across[q].wait()
        at = cols(c * half + q * size, size)
        whole_out[:, at] = (h_out[q].astype(F32) + h_in[q].astype(F32)).astype(BF16)
        beside.append(push(2 + 2 * pieces + q, whole_out.at[:, at], whole_out.at[:, at], mate))
    for step in range(n - 1):
        for way in ways:
            for w in range(3):
                @pl.when(sends(step, way))
                def _():
                    hop(w, step, way).wait_send()

            @pl.when(sum_goes(step, way))
            def _():
                sum_copy(step, way, False).wait_send()
    for copy in small:
        copy.wait()
    here = n_own[...]
    for i in range(n - 1):
        here = here + n_in[i]
    there = n_in[n - 1]
    for i in range(n, 2 * n - 1):
        there = there + n_in[i]
    norms[...] = jnp.concatenate(
        [jnp.where(r == 0, here, there), jnp.where(r == 0, there, here)], axis=1
    )
    swap.wait()
    down_grad[pl.ds(pl.multiple_of((1 - r) * units, 16), units), :] = s_other[...]
    for copy in beside:
        copy.wait()
    input_grad[...] = whole_out[...]


def write_kernel(flow, shard, rows, input_grad, down_grad, norms):
    input_grad[...] = flow[...]
    down_grad[...] = shard[...].astype(F32)
    norms[...] = rows[0]


def split_units(n, tokens, gate_weight, up_weight, down_weight, out_grad):
    rows, depth = tokens.shape
    width, both = gate_weight.shape
    units = both // 2
    start = lax.axis_index("rep") * units
    gate = lax.dynamic_slice_in_dim(gate_weight, start, units, 1).T
    up = lax.dynamic_slice_in_dim(up_weight, start, units, 1).T
    anywhere = pl.BlockSpec(memory_space=pl.ANY)
    vmem = pl.BlockSpec(memory_space=pltpu.VMEM)
    dma = pltpu.SemaphoreType.DMA
    half, pieces = depth // 2, 4
    piece = (pieces, rows, half // pieces)
    peers = 2 * n - 1
    scratch = [((units, depth), BF16)] * 3 + [((2 * rows, depth), BF16)] * 2
    scratch += [((2 * rows, units), F32)] * 3 + [((2 * rows, units), BF16)] * 2
    scratch += [((units, depth), BF16)] + [((2, n - 1, units, width), BF16)] * 2
    scratch += [((2, rows, half), BF16)] * 2 + [(piece, F32)] + [(piece, BF16)] * 4
    scratch += [((rows, depth), BF16)] + [((units, width), BF16)] * 2
    scratch += [((8, units), F32), ((peers, 8, units), F32)]
    input_grad, down_grad, norms = pl.pallas_call(
        functools.partial(block_kernel, n),
        out_shape=[
            jax.ShapeDtypeStruct((rows, depth), BF16),
            jax.ShapeDtypeStruct((both, width), BF16),
            jax.ShapeDtypeStruct((8, both), F32),
        ],
        in_specs=[vmem] * 2 + [anywhere] * 3,
        out_specs=[vmem] * 3,
        scratch_shapes=[pltpu.VMEM(shape, kind) for shape, kind in scratch] + [
            dma((2, 3, n - 1)), dma((2, 3, n - 1)), dma((2, n - 1)), dma((2, n - 1)),
            dma((2,)), dma((2,)), dma((5,)), dma((2 + 3 * pieces,)), dma((2 + 3 * pieces,)),
            dma, dma, dma((peers,)), dma((peers,)),
        ],
        compiler_params=pltpu.CompilerParams(collective_id=0, has_side_effects=True),
        name="block",
    )(gate, up, down_weight, tokens, out_grad)
    return tuple(pl.pallas_call(
        write_kernel,
        out_shape=[
            jax.ShapeDtypeStruct((rows, depth), BF16),
            jax.ShapeDtypeStruct((both, width), F32),
            jax.ShapeDtypeStruct((both,), F32),
        ],
        in_specs=[vmem] * 3,
        out_specs=[vmem] * 3,
        name="write",
    )(input_grad, down_grad, norms))


def whole_units(tokens, gate_weight, up_weight, down_weight, out_grad):
    down_full = lax.all_gather(down_weight, "fs", axis=1, tiled=True)
    gate_full = lax.all_gather(gate_weight, "fs", axis=0, tiled=True)
    up_full = lax.all_gather(up_weight, "fs", axis=0, tiled=True)
    gate_pre = jnp.dot(tokens, gate_full, preferred_element_type=F32)
    up_pre = jnp.dot(tokens, up_full, preferred_element_type=F32)
    sigma = jax.nn.sigmoid(gate_pre)
    activated = gate_pre * sigma
    hidden = (activated * up_pre).astype(BF16)
    hid_grad = contract_last(out_grad, down_full)
    up_grad = (hid_grad * activated).astype(BF16)
    gate_grad = (hid_grad * up_pre * sigma * (1.0 + gate_pre * (1.0 - sigma))).astype(BF16)
    partial_value = contract_last(gate_grad, gate_full) + contract_last(up_grad, up_full)
    input_grad = lax.psum(partial_value.astype(BF16), "tp")
    columns = lax.all_to_all(out_grad, "fs", split_axis=1, concat_axis=0, tiled=True)
    shard = contract_first(lax.all_gather(hidden, "fs", axis=0, tiled=True), columns)
    shard = lax.psum(shard.astype(BF16), "rep").astype(F32)
    norms = lax.psum(jnp.sum(shard * shard, axis=1), "fs")
    return (input_grad, shard, norms)


def solution(mesh):
    n, rep, tp = mesh.shape["fs"], mesh.shape["rep"], mesh.shape["tp"]

    def on_device(tokens, gate_weight, up_weight, down_weight, out_grad):
        width, both = gate_weight.shape
        if rep == 2 and tp == 4 and 2 <= n <= 4 and both % 32 == 0 and width % 128 == 0:
            return split_units(n, tokens, gate_weight, up_weight, down_weight, out_grad)
        return whole_units(tokens, gate_weight, up_weight, down_weight, out_grad)

    return jax.shard_map(
        on_device,
        mesh=mesh,
        in_specs=(
            P(("rep", "fs"), None),
            P("fs", "tp"),
            P("fs", "tp"),
            P("tp", "fs"),
            P(("rep", "fs"), None),
        ),
        out_specs=(P(("rep", "fs"), None), P("tp", "fs"), P("tp")),
        check_vma=False,
    )
```

```python
import functools

import jax
import jax.numpy as jnp
from jax import lax
from jax.experimental import pallas as pl
from jax.experimental.pallas import tpu as pltpu
from jax.sharding import PartitionSpec as P

MESH = pl.DeviceIdType.MESH
BF16 = jnp.bfloat16
F32 = jnp.float32


def contract_last(left, right):
    return lax.dot_general(left, right, (((1,), (1,)), ((), ())), preferred_element_type=F32)


def contract_first(left, right):
    return lax.dot_general(left, right, (((0,), (0,)), ((), ())), preferred_element_type=F32)


def block_kernel(
    n, gate, up, down, tokens, grad, input_grad, down_grad, norms,
    gate_all, up_all, down_all, tokens_all, grad_all,
    gate_pre, up_pre, hid, gate_grad, up_grad, part, p_in, p_out,
    f_out, f_in, g_own, g_out, g_in, h_out, h_in, whole_out, s_own, s_other, n_own, n_in,
    w_send, w_recv, p_send, p_recv, pair_send, pair_recv, own_sem, g_send, g_recv,
    s_send, s_recv, n_send, n_recv,
):
    f = lax.axis_index("fs")
    r = lax.axis_index("rep")
    t = lax.axis_index("tp")
    c, x = lax.rem(t, 2), t // 2
    mate, far = {"tp": x * 2 + 1 - c}, {"tp": (1 - x) * 2 + c}
    pair = {"rep": 1 - r}
    rows, depth = tokens.shape
    units, width = gate.shape
    half, strip = depth // 2, width // 2
    pieces = g_out.shape[0]
    size = half // pieces
    down_half = down.at[pl.ds(pl.multiple_of(r * units, 16), units)]

    barrier = pltpu.get_barrier_semaphore()
    peers = [{"rep": lax.rem(r + a, 2), "fs": lax.rem(f + k, n)}
             for a in range(2) for k in range(n) if a or k]
    for peer in peers + [mate, far]:
        pl.semaphore_signal(barrier, inc=1, device_id=peer, device_id_type=MESH)
    pl.semaphore_wait(barrier, 2 * n + 1)

    def cols(start, size):
        return pl.ds(pl.multiple_of(start, size), size)

    def remote(src, dst, send, recv, peer):
        return pltpu.make_async_remote_copy(
            src_ref=src, dst_ref=dst, send_sem=send, recv_sem=recv,
            device_id=peer, device_id_type=MESH,
        )

    shards = ((gate, gate_all), (up, up_all), (down_half, down_all))
    ways = (1, 0)

    def hop(w, step, way, arriving=False):
        own, whole = shards[w]
        sign = 1 if way else -1
        owner = f - sign * (step + 1 if arriving else step)
        place = whole.at[:, cols(owner * width, width)]
        return remote(
            own if step == 0 and not arriving else place, place,
            w_send.at[way, w, step], w_recv.at[way, w, step],
            {"fs": f - sign if arriving else f + sign},
        )

    def sends(step, way):
        return (f < n - 1) & (f >= step) if way else (f > 0) & (f + step <= n - 1)

    def receives(step, way):
        return f - 1 - step >= 0 if way else f + 1 + step <= n - 1

    def forward(w, step):
        for way in ways:
            @pl.when(sends(step, way))
            def _():
                hop(w, step, way).start()

    def arrive(w, step):
        for way in ways:
            @pl.when(receives(step, way))
            def _():
                hop(w, step, way, True).wait_recv()

    for w in range(2):
        forward(w, 0)
    pairs = []
    for i, (own, whole) in enumerate(((tokens, tokens_all), (grad, grad_all))):
        copy = remote(own, whole.at[pl.ds(rows, rows)], pair_send.at[i], pair_recv.at[i], pair)
        copy.start()
        pairs.append(copy)
    local = []
    for i, (own, place) in enumerate((
        (tokens, tokens_all.at[pl.ds(0, rows)]),
        (grad, grad_all.at[pl.ds(0, rows)]),
        (gate, gate_all.at[:, cols(f * width, width)]),
        (up, up_all.at[:, cols(f * width, width)]),
        (down_half, down_all.at[:, cols(f * width, width)]),
    )):
        copy = pltpu.make_async_copy(own, place, own_sem.at[i])
        copy.start()
        local.append(copy)

    for step in range(n - 1):
        if step == n - 2:
            forward(2, 0)
        for w in range(2):
            arrive(w, step)
            if step + 1 < n - 1:
                forward(w, step + 1)
    for copy in pairs + local:
        copy.wait()

    for b in range(2):
        span = pl.ds(b * rows, rows)
        gate_pre[span] = contract_last(tokens_all[span], gate_all[...])
        up_pre[span] = contract_last(tokens_all[span], up_all[...])

    def relay_down(step):
        arrive(2, step)
        if step + 1 < n - 1:
            forward(2, step + 1)

    relay_down(0)
    pre, raw = gate_pre[...], up_pre[...]
    sigma = jax.nn.sigmoid(pre)
    hidden = (pre * sigma * raw).astype(BF16)
    gate_pre[...] = pre * sigma
    up_pre[...] = raw * sigma * (1.0 + pre * (1.0 - sigma))
    for k in range(n):
        at = pl.ds(k * width, width)
        part[:, at] = contract_first(hidden, grad_all[:, at]).astype(BF16)

    def sum_goes(step, way):
        return f <= n - 2 - step if way else f >= step + 1

    def sum_comes(step, way):
        return (f >= 1) & (f <= n - 1 - step) if way else (f <= n - 2) & (f >= step)

    def lanes(k, base=0):
        return pl.ds(base * width + k * strip, strip)

    def sum_copy(step, way, k, first):
        target = n - 1 - step if way else step
        return remote(
            part.at[:, lanes(k, target)] if first else p_out.at[way, step, :, lanes(k)],
            p_in.at[way, step, :, lanes(k)], p_send.at[way, step, k], p_recv.at[way, step, k],
            {"fs": f + 1 if way else f - 1},
        )

    def at_end(way):
        return f == 0 if way else f == n - 1

    for step in range(n - 1):
        for way in ways:
            @pl.when(at_end(way))
            def _():
                for k in range(2):
                    sum_copy(step, way, k, True).start()

    def relay_sum(step, hops, k):
        for way in ways:
            target = n - 1 - step if way else step
            here = f == hops if way else f == n - 1 - hops

            @pl.when(sum_comes(step, way) & here)
            def _():
                sum_copy(step, way, k, False).wait_recv()

            @pl.when(sum_comes(step, way) & sum_goes(step, way) & here)
            def _():
                p_out[way, step, :, lanes(k)] = (
                    part[:, lanes(k, target)].astype(F32) + p_in[way, step, :, lanes(k)].astype(F32)
                ).astype(BF16)
                sum_copy(step, way, k, False).start()

    def relay_sums(when, k):
        for step in range(n - 1):
            hops = when - step
            if 1 <= hops <= n - 1 - step:
                relay_sum(step, hops, k)

    def add_shard(owner):
        at = cols(owner * width, width)
        hid[...] += contract_last(grad_all[:, at], down_all[:, at])

    def add_shards(step):
        for way in ways:
            @pl.when(receives(step, way))
            def _():
                add_shard(f - 1 - step if way else f + 1 + step)

    mine = cols(f * width, width)
    hid[...] = contract_last(grad_all[:, mine], down_all[:, mine])
    add_shards(0)
    for step in range(1, n - 1):
        relay_down(step)
        add_shards(step)
        if step == 1:
            relay_sums(1, 0)
            relay_sums(1, 1)
    if n == 2:
        relay_sums(1, 0)
        relay_sums(1, 1)

    for b in range(2):
        span = pl.ds(b * rows, rows)
        up_grad[span] = (hid[span] * gate_pre[span]).astype(BF16)
        gate_grad[span] = (hid[span] * up_pre[span]).astype(BF16)

    def flow(b, at):
        span = pl.ds(b * rows, rows)
        return (
            jnp.dot(gate_grad[span], gate_all[:, at], preferred_element_type=F32)
            + jnp.dot(up_grad[span], up_all[:, at], preferred_element_type=F32)
        )

    def push(i, src, dst, peer):
        copy = remote(src, dst, g_send.at[i], g_recv.at[i], peer)
        copy.start()
        return copy

    cross = {}
    for b in (1, 0):
        f_out[b] = flow(b, cols((1 - c) * half, half)).astype(BF16)
        cross[b] = push(b, f_out.at[b], f_in.at[b], mate)
    over = []
    for b in (1, 0):
        if b == 0:
            for k in range(2):
                relay_sums(2, k)
        kept = flow(b, cols(c * half, half))
        cross[b].wait()
        kept = kept + f_in[b].astype(F32)
        for q in range(pieces):
            piece = kept[:, q * size:(q + 1) * size]
            if b == 1:
                g_out[q] = piece.astype(BF16)
                over.append(push(2 + q, g_out.at[q], g_in.at[q], pair))
            else:
                g_own[q] = piece
    across = []
    for q in range(pieces):
        over[q].wait()
        h_out[q] = (g_own[q] + g_in[q].astype(F32)).astype(BF16)
        across.append(push(2 + pieces + q, h_out.at[q], h_in.at[q], far))
    swaps = []
    for k in range(2):
        for when in range(3, n):
            relay_sums(when, k)

        def finish(way):
            step = n - 1 - f if way else f
            return p_in[way, lax.rem(step, n - 1), :, lanes(k)].astype(F32)

        at = pl.ds(pl.multiple_of(f * width + k * strip, strip), strip)
        s_sum = part[:, at].astype(F32)
        s_sum = s_sum + jnp.where(f > 0, finish(1), 0.0) + jnp.where(f < n - 1, finish(0), 0.0)
        s_own[:, lanes(k)] = s_sum.astype(BF16)
        copy = remote(
            s_own.at[:, lanes(k)], s_other.at[:, lanes(k)], s_send.at[k], s_recv.at[k], pair
        )
        copy.start()
        swaps.append(copy)
    kept = s_own[...].astype(F32)
    down_grad[pl.ds(pl.multiple_of(r * units, 16), units), :] = s_own[...]
    n_own[...] = lax.dot_general(
        jnp.ones((8, width), F32), kept * kept, (((1,), (1,)), ((), ())),
        precision=lax.Precision.HIGHEST, preferred_element_type=F32,
    )
    small = []
    for i, peer in enumerate(peers):
        copy = remote(n_own, n_in.at[i], n_send.at[i], n_recv.at[i], peer)
        copy.start()
        small.append(copy)
    beside = []
    for q in range(pieces):
        across[q].wait()
        at = cols(c * half + q * size, size)
        whole_out[:, at] = (h_out[q].astype(F32) + h_in[q].astype(F32)).astype(BF16)
        beside.append(push(2 + 2 * pieces + q, whole_out.at[:, at], whole_out.at[:, at], mate))
    for step in range(n - 1):
        for way in ways:
            for w in range(3):
                @pl.when(sends(step, way))
                def _():
                    hop(w, step, way).wait_send()

            @pl.when(sum_goes(step, way))
            def _():
                for k in range(2):
                    sum_copy(step, way, k, False).wait_send()
    for copy in small:
        copy.wait()
    here = n_own[...]
    for i in range(n - 1):
        here = here + n_in[i]
    there = n_in[n - 1]
    for i in range(n, 2 * n - 1):
        there = there + n_in[i]
    norms[...] = jnp.concatenate(
        [jnp.where(r == 0, here, there), jnp.where(r == 0, there, here)], axis=1
    )
    for copy in swaps:
        copy.wait()
    down_grad[pl.ds(pl.multiple_of((1 - r) * units, 16), units), :] = s_other[...]
    for copy in beside:
        copy.wait()
    input_grad[...] = whole_out[...]


def write_kernel(flow, shard, rows, input_grad, down_grad, norms):
    input_grad[...] = flow[...]
    down_grad[...] = shard[...].astype(F32)
    norms[...] = rows[0]


def split_units(n, tokens, gate_weight, up_weight, down_weight, out_grad):
    rows, depth = tokens.shape
    width, both = gate_weight.shape
    units = both // 2
    start = lax.axis_index("rep") * units
    gate = lax.dynamic_slice_in_dim(gate_weight, start, units, 1).T
    up = lax.dynamic_slice_in_dim(up_weight, start, units, 1).T
    anywhere = pl.BlockSpec(memory_space=pl.ANY)
    vmem = pl.BlockSpec(memory_space=pltpu.VMEM)
    dma = pltpu.SemaphoreType.DMA
    half, pieces = depth // 2, 4
    piece = (pieces, rows, half // pieces)
    peers = 2 * n - 1
    scratch = [((units, depth), BF16)] * 3 + [((2 * rows, depth), BF16)] * 2
    scratch += [((2 * rows, units), F32)] * 3 + [((2 * rows, units), BF16)] * 2
    scratch += [((units, depth), BF16)] + [((2, n - 1, units, width), BF16)] * 2
    scratch += [((2, rows, half), BF16)] * 2 + [(piece, F32)] + [(piece, BF16)] * 4
    scratch += [((rows, depth), BF16)] + [((units, width), BF16)] * 2
    scratch += [((8, units), F32), ((peers, 8, units), F32)]
    input_grad, down_grad, norms = pl.pallas_call(
        functools.partial(block_kernel, n),
        out_shape=[
            jax.ShapeDtypeStruct((rows, depth), BF16),
            jax.ShapeDtypeStruct((both, width), BF16),
            jax.ShapeDtypeStruct((8, both), F32),
        ],
        in_specs=[vmem] * 2 + [anywhere] * 3,
        out_specs=[vmem] * 3,
        scratch_shapes=[pltpu.VMEM(shape, kind) for shape, kind in scratch] + [
            dma((2, 3, n - 1)), dma((2, 3, n - 1)), dma((2, n - 1, 2)), dma((2, n - 1, 2)),
            dma((2,)), dma((2,)), dma((5,)), dma((2 + 3 * pieces,)), dma((2 + 3 * pieces,)),
            dma((2,)), dma((2,)), dma((peers,)), dma((peers,)),
        ],
        compiler_params=pltpu.CompilerParams(collective_id=0, has_side_effects=True),
        name="block",
    )(gate, up, down_weight, tokens, out_grad)
    return tuple(pl.pallas_call(
        write_kernel,
        out_shape=[
            jax.ShapeDtypeStruct((rows, depth), BF16),
            jax.ShapeDtypeStruct((both, width), F32),
            jax.ShapeDtypeStruct((both,), F32),
        ],
        in_specs=[vmem] * 3,
        out_specs=[vmem] * 3,
        name="write",
    )(input_grad, down_grad, norms))


def whole_units(tokens, gate_weight, up_weight, down_weight, out_grad):
    down_full = lax.all_gather(down_weight, "fs", axis=1, tiled=True)
    gate_full = lax.all_gather(gate_weight, "fs", axis=0, tiled=True)
    up_full = lax.all_gather(up_weight, "fs", axis=0, tiled=True)
    gate_pre = jnp.dot(tokens, gate_full, preferred_element_type=F32)
    up_pre = jnp.dot(tokens, up_full, preferred_element_type=F32)
    sigma = jax.nn.sigmoid(gate_pre)
    activated = gate_pre * sigma
    hidden = (activated * up_pre).astype(BF16)
    hid_grad = contract_last(out_grad, down_full)
    up_grad = (hid_grad * activated).astype(BF16)
    gate_grad = (hid_grad * up_pre * sigma * (1.0 + gate_pre * (1.0 - sigma))).astype(BF16)
    partial_value = contract_last(gate_grad, gate_full) + contract_last(up_grad, up_full)
    input_grad = lax.psum(partial_value.astype(BF16), "tp")
    columns = lax.all_to_all(out_grad, "fs", split_axis=1, concat_axis=0, tiled=True)
    shard = contract_first(lax.all_gather(hidden, "fs", axis=0, tiled=True), columns)
    shard = lax.psum(shard.astype(BF16), "rep").astype(F32)
    norms = lax.psum(jnp.sum(shard * shard, axis=1), "fs")
    return (input_grad, shard, norms)


def solution(mesh):
    n, rep, tp = mesh.shape["fs"], mesh.shape["rep"], mesh.shape["tp"]

    def on_device(tokens, gate_weight, up_weight, down_weight, out_grad):
        width, both = gate_weight.shape
        if rep == 2 and tp == 4 and 2 <= n <= 4 and both % 32 == 0 and width % 256 == 0:
            return split_units(n, tokens, gate_weight, up_weight, down_weight, out_grad)
        return whole_units(tokens, gate_weight, up_weight, down_weight, out_grad)

    return jax.shard_map(
        on_device,
        mesh=mesh,
        in_specs=(
            P(("rep", "fs"), None),
            P("fs", "tp"),
            P("fs", "tp"),
            P("tp", "fs"),
            P(("rep", "fs"), None),
        ),
        out_specs=(P(("rep", "fs"), None), P("tp", "fs"), P("tp")),
        check_vma=False,
    )
```

```python
import functools

import jax
import jax.numpy as jnp
from jax import lax
from jax.experimental import pallas as pl
from jax.experimental.pallas import tpu as pltpu
from jax.sharding import PartitionSpec as P

MESH = pl.DeviceIdType.MESH
BF16 = jnp.bfloat16
F32 = jnp.float32


def contract_last(left, right):
    return lax.dot_general(left, right, (((1,), (1,)), ((), ())), preferred_element_type=F32)


def contract_first(left, right):
    return lax.dot_general(left, right, (((0,), (0,)), ((), ())), preferred_element_type=F32)


def block_kernel(
    n, gate, up, down, tokens, grad, input_grad, down_grad, norms,
    gate_all, up_all, down_all, tokens_all, grad_all,
    gate_pre, up_pre, hid, gate_grad, up_grad, part, p_in, p_out,
    f_out, f_in, g_own, g_out, g_in, h_out, h_in, whole_out, s_own, s_other, n_own, n_in,
    w_send, w_recv, p_send, p_recv, pair_send, pair_recv, own_sem, g_send, g_recv,
    s_send, s_recv, n_send, n_recv,
):
    f = lax.axis_index("fs")
    r = lax.axis_index("rep")
    t = lax.axis_index("tp")
    c, x = lax.rem(t, 2), t // 2
    mate, far = {"tp": x * 2 + 1 - c}, {"tp": (1 - x) * 2 + c}
    pair = {"rep": 1 - r}
    rows, depth = tokens.shape
    units, width = gate.shape
    half, strip = depth // 2, width // 2
    pieces = g_out.shape[0]
    size = half // pieces
    down_half = down.at[pl.ds(pl.multiple_of(r * units, 16), units)]

    barrier = pltpu.get_barrier_semaphore()
    peers = [{"rep": lax.rem(r + a, 2), "fs": lax.rem(f + k, n)}
             for a in range(2) for k in range(n) if a or k]
    for peer in peers + [mate, far]:
        pl.semaphore_signal(barrier, inc=1, device_id=peer, device_id_type=MESH)
    pl.semaphore_wait(barrier, 2 * n + 1)

    def cols(start, size):
        return pl.ds(pl.multiple_of(start, size), size)

    def remote(src, dst, send, recv, peer):
        return pltpu.make_async_remote_copy(
            src_ref=src, dst_ref=dst, send_sem=send, recv_sem=recv,
            device_id=peer, device_id_type=MESH,
        )

    shards = ((gate, gate_all), (up, up_all), (down_half, down_all))
    ways = (1, 0)

    def hop(w, step, way, arriving=False):
        own, whole = shards[w]
        sign = 1 if way else -1
        owner = f - sign * (step + 1 if arriving else step)
        place = whole.at[:, cols(owner * width, width)]
        return remote(
            own if step == 0 and not arriving else place, place,
            w_send.at[way, w, step], w_recv.at[way, w, step],
            {"fs": f - sign if arriving else f + sign},
        )

    def sends(step, way):
        return (f < n - 1) & (f >= step) if way else (f > 0) & (f + step <= n - 1)

    def receives(step, way):
        return f - 1 - step >= 0 if way else f + 1 + step <= n - 1

    def forward(w, step):
        for way in ways:
            @pl.when(sends(step, way))
            def _():
                hop(w, step, way).start()

    def arrive(w, step):
        for way in ways:
            @pl.when(receives(step, way))
            def _():
                hop(w, step, way, True).wait_recv()

    for w in range(2):
        forward(w, 0)
    pairs = []
    for i, (own, whole) in enumerate(((tokens, tokens_all), (grad, grad_all))):
        copy = remote(own, whole.at[pl.ds(rows, rows)], pair_send.at[i], pair_recv.at[i], pair)
        copy.start()
        pairs.append(copy)
    local = []
    for i, (own, place) in enumerate((
        (tokens, tokens_all.at[pl.ds(0, rows)]),
        (grad, grad_all.at[pl.ds(0, rows)]),
        (gate, gate_all.at[:, cols(f * width, width)]),
        (up, up_all.at[:, cols(f * width, width)]),
        (down_half, down_all.at[:, cols(f * width, width)]),
    )):
        copy = pltpu.make_async_copy(own, place, own_sem.at[i])
        copy.start()
        local.append(copy)

    for step in range(n - 1):
        if step == n - 2:
            forward(2, 0)
        for w in range(2):
            arrive(w, step)
            if step + 1 < n - 1:
                forward(w, step + 1)
    for copy in pairs + local:
        copy.wait()

    for b in range(2):
        span = pl.ds(b * rows, rows)
        gate_pre[span] = contract_last(tokens_all[span], gate_all[...])
        up_pre[span] = contract_last(tokens_all[span], up_all[...])

    def relay_down(step):
        arrive(2, step)
        if step + 1 < n - 1:
            forward(2, step + 1)

    relay_down(0)
    pre, raw = gate_pre[...], up_pre[...]
    sigma = jax.nn.sigmoid(pre)
    hidden = (pre * sigma * raw).astype(BF16)
    gate_pre[...] = pre * sigma
    up_pre[...] = raw * sigma * (1.0 + pre * (1.0 - sigma))
    for k in range(n):
        at = pl.ds(k * width, width)
        part[:, at] = contract_first(hidden, grad_all[:, at]).astype(BF16)

    def sum_goes(step, way):
        return f <= n - 2 - step if way else f >= step + 1

    def sum_comes(step, way):
        return (f >= 1) & (f <= n - 1 - step) if way else (f <= n - 2) & (f >= step)

    def lanes(k, base=0):
        return pl.ds(base * width + k * strip, strip)

    def sum_copy(step, way, k, first):
        target = n - 1 - step if way else step
        return remote(
            part.at[:, lanes(k, target)] if first else p_out.at[way, step, :, lanes(k)],
            p_in.at[way, step, :, lanes(k)], p_send.at[way, step, k], p_recv.at[way, step, k],
            {"fs": f + 1 if way else f - 1},
        )

    def at_end(way):
        return f == 0 if way else f == n - 1

    for step in range(n - 1):
        for way in ways:
            @pl.when(at_end(way))
            def _():
                for k in range(2):
                    sum_copy(step, way, k, True).start()

    def relay_sum(step, hops, k):
        for way in ways:
            target = n - 1 - step if way else step
            here = f == hops if way else f == n - 1 - hops

            @pl.when(sum_comes(step, way) & here)
            def _():
                sum_copy(step, way, k, False).wait_recv()

            @pl.when(sum_comes(step, way) & sum_goes(step, way) & here)
            def _():
                p_out[way, step, :, lanes(k)] = (
                    part[:, lanes(k, target)].astype(F32) + p_in[way, step, :, lanes(k)].astype(F32)
                ).astype(BF16)
                sum_copy(step, way, k, False).start()

    def relay_sums(when, k):
        for step in range(n - 1):
            hops = when - step
            if 1 <= hops <= n - 1 - step:
                relay_sum(step, hops, k)

    def add_shard(owner):
        at = cols(owner * width, width)
        hid[...] += contract_last(grad_all[:, at], down_all[:, at])

    def add_shards(step):
        for way in ways:
            @pl.when(receives(step, way))
            def _():
                add_shard(f - 1 - step if way else f + 1 + step)

    mine = cols(f * width, width)
    hid[...] = contract_last(grad_all[:, mine], down_all[:, mine])
    add_shards(0)
    for step in range(1, n - 1):
        relay_down(step)
        add_shards(step)
        if step == 1:
            relay_sums(1, 0)
            relay_sums(1, 1)
    if n == 2:
        relay_sums(1, 0)
        relay_sums(1, 1)

    for b in range(2):
        span = pl.ds(b * rows, rows)
        up_grad[span] = (hid[span] * gate_pre[span]).astype(BF16)
        gate_grad[span] = (hid[span] * up_pre[span]).astype(BF16)

    def flow(b, at):
        span = pl.ds(b * rows, rows)
        return (
            jnp.dot(gate_grad[span], gate_all[:, at], preferred_element_type=F32)
            + jnp.dot(up_grad[span], up_all[:, at], preferred_element_type=F32)
        )

    def push(i, src, dst, peer):
        copy = remote(src, dst, g_send.at[i], g_recv.at[i], peer)
        copy.start()
        return copy

    cross = {}
    for b in (1, 0):
        f_out[b] = flow(b, cols((1 - c) * half, half)).astype(BF16)
        cross[b] = push(b, f_out.at[b], f_in.at[b], mate)
    over = []
    for b in (1, 0):
        if b == 0:
            for k in range(2):
                relay_sums(2, k)
        kept = flow(b, cols(c * half, half))
        cross[b].wait()
        kept = kept + f_in[b].astype(F32)
        for q in range(pieces):
            piece = kept[:, q * size:(q + 1) * size]
            if b == 1:
                g_out[q] = piece.astype(BF16)
                over.append(push(2 + q, g_out.at[q], g_in.at[q], pair))
            else:
                g_own[q] = piece
    across = []
    for q in range(pieces):
        over[q].wait()
        h_out[q] = (g_own[q] + g_in[q].astype(F32)).astype(BF16)
        across.append(push(2 + pieces + q, h_out.at[q], h_in.at[q], far))
    swaps = []
    for k in range(2):
        for when in range(3, n):
            relay_sums(when, k)

        def finish(way):
            step = n - 1 - f if way else f
            return p_in[way, lax.rem(step, n - 1), :, lanes(k)].astype(F32)

        at = pl.ds(pl.multiple_of(f * width + k * strip, strip), strip)
        s_sum = part[:, at].astype(F32)
        s_sum = s_sum + jnp.where(f > 0, finish(1), 0.0) + jnp.where(f < n - 1, finish(0), 0.0)
        s_own[:, lanes(k)] = s_sum.astype(BF16)
        copy = remote(
            s_own.at[:, lanes(k)], s_other.at[:, lanes(k)], s_send.at[k], s_recv.at[k], pair
        )
        copy.start()
        swaps.append(copy)
    kept = s_own[...].astype(F32)
    down_grad[pl.ds(pl.multiple_of(r * units, 16), units), :] = s_own[...]
    n_own[...] = lax.dot_general(
        jnp.ones((8, width), F32), kept * kept, (((1,), (1,)), ((), ())),
        precision=lax.Precision.HIGHEST, preferred_element_type=F32,
    )
    small = []
    for i, peer in enumerate(peers):
        copy = remote(n_own, n_in.at[i], n_send.at[i], n_recv.at[i], peer)
        copy.start()
        small.append(copy)
    beside = []
    for q in range(pieces):
        across[q].wait()
        at = cols(c * half + q * size, size)
        whole_out[:, at] = (h_out[q].astype(F32) + h_in[q].astype(F32)).astype(BF16)
        beside.append(push(2 + 2 * pieces + q, whole_out.at[:, at], whole_out.at[:, at], mate))
    for step in range(n - 1):
        for way in ways:
            for w in range(3):
                @pl.when(sends(step, way))
                def _():
                    hop(w, step, way).wait_send()

            @pl.when(sum_goes(step, way))
            def _():
                for k in range(2):
                    sum_copy(step, way, k, False).wait_send()
    for copy in small:
        copy.wait()
    here = n_own[...]
    for i in range(n - 1):
        here = here + n_in[i]
    there = n_in[n - 1]
    for i in range(n, 2 * n - 1):
        there = there + n_in[i]
    norms[...] = jnp.concatenate(
        [jnp.where(r == 0, here, there), jnp.where(r == 0, there, here)], axis=1
    )
    for copy in swaps:
        copy.wait()
    down_grad[pl.ds(pl.multiple_of((1 - r) * units, 16), units), :] = s_other[...]
    for copy in beside:
        copy.wait()
    input_grad[...] = whole_out[...]


def write_kernel(flow, shard, rows, input_grad, down_grad, norms):
    input_grad[...] = flow[...]
    down_grad[...] = shard[...].astype(F32)
    norms[...] = rows[0]


def split_units(n, tokens, gate_weight, up_weight, down_weight, out_grad):
    rows, depth = tokens.shape
    width, both = gate_weight.shape
    units = both // 2
    start = lax.axis_index("rep") * units
    gate = lax.dynamic_slice_in_dim(gate_weight, start, units, 1).T
    up = lax.dynamic_slice_in_dim(up_weight, start, units, 1).T
    anywhere = pl.BlockSpec(memory_space=pl.ANY)
    vmem = pl.BlockSpec(memory_space=pltpu.VMEM)
    dma = pltpu.SemaphoreType.DMA
    half, pieces = depth // 2, 8
    piece = (pieces, rows, half // pieces)
    peers = 2 * n - 1
    scratch = [((units, depth), BF16)] * 3 + [((2 * rows, depth), BF16)] * 2
    scratch += [((2 * rows, units), F32)] * 3 + [((2 * rows, units), BF16)] * 2
    scratch += [((units, depth), BF16)] + [((2, n - 1, units, width), BF16)] * 2
    scratch += [((2, rows, half), BF16)] * 2 + [(piece, F32)] + [(piece, BF16)] * 4
    scratch += [((rows, depth), BF16)] + [((units, width), BF16)] * 2
    scratch += [((8, units), F32), ((peers, 8, units), F32)]
    input_grad, down_grad, norms = pl.pallas_call(
        functools.partial(block_kernel, n),
        out_shape=[
            jax.ShapeDtypeStruct((rows, depth), BF16),
            jax.ShapeDtypeStruct((both, width), BF16),
            jax.ShapeDtypeStruct((8, both), F32),
        ],
        in_specs=[vmem] * 2 + [anywhere] * 3,
        out_specs=[vmem] * 3,
        scratch_shapes=[pltpu.VMEM(shape, kind) for shape, kind in scratch] + [
            dma((2, 3, n - 1)), dma((2, 3, n - 1)), dma((2, n - 1, 2)), dma((2, n - 1, 2)),
            dma((2,)), dma((2,)), dma((5,)), dma((2 + 3 * pieces,)), dma((2 + 3 * pieces,)),
            dma((2,)), dma((2,)), dma((peers,)), dma((peers,)),
        ],
        compiler_params=pltpu.CompilerParams(collective_id=0, has_side_effects=True),
        name="block",
    )(gate, up, down_weight, tokens, out_grad)
    return tuple(pl.pallas_call(
        write_kernel,
        out_shape=[
            jax.ShapeDtypeStruct((rows, depth), BF16),
            jax.ShapeDtypeStruct((both, width), F32),
            jax.ShapeDtypeStruct((both,), F32),
        ],
        in_specs=[vmem] * 3,
        out_specs=[vmem] * 3,
        name="write",
    )(input_grad, down_grad, norms))


def whole_units(tokens, gate_weight, up_weight, down_weight, out_grad):
    down_full = lax.all_gather(down_weight, "fs", axis=1, tiled=True)
    gate_full = lax.all_gather(gate_weight, "fs", axis=0, tiled=True)
    up_full = lax.all_gather(up_weight, "fs", axis=0, tiled=True)
    gate_pre = jnp.dot(tokens, gate_full, preferred_element_type=F32)
    up_pre = jnp.dot(tokens, up_full, preferred_element_type=F32)
    sigma = jax.nn.sigmoid(gate_pre)
    activated = gate_pre * sigma
    hidden = (activated * up_pre).astype(BF16)
    hid_grad = contract_last(out_grad, down_full)
    up_grad = (hid_grad * activated).astype(BF16)
    gate_grad = (hid_grad * up_pre * sigma * (1.0 + gate_pre * (1.0 - sigma))).astype(BF16)
    partial_value = contract_last(gate_grad, gate_full) + contract_last(up_grad, up_full)
    input_grad = lax.psum(partial_value.astype(BF16), "tp")
    columns = lax.all_to_all(out_grad, "fs", split_axis=1, concat_axis=0, tiled=True)
    shard = contract_first(lax.all_gather(hidden, "fs", axis=0, tiled=True), columns)
    shard = lax.psum(shard.astype(BF16), "rep").astype(F32)
    norms = lax.psum(jnp.sum(shard * shard, axis=1), "fs")
    return (input_grad, shard, norms)


def solution(mesh):
    n, rep, tp = mesh.shape["fs"], mesh.shape["rep"], mesh.shape["tp"]

    def on_device(tokens, gate_weight, up_weight, down_weight, out_grad):
        width, both = gate_weight.shape
        if rep == 2 and tp == 4 and 2 <= n <= 4 and both % 32 == 0 and width % 256 == 0:
            return split_units(n, tokens, gate_weight, up_weight, down_weight, out_grad)
        return whole_units(tokens, gate_weight, up_weight, down_weight, out_grad)

    return jax.shard_map(
        on_device,
        mesh=mesh,
        in_specs=(
            P(("rep", "fs"), None),
            P("fs", "tp"),
            P("fs", "tp"),
            P("tp", "fs"),
            P(("rep", "fs"), None),
        ),
        out_specs=(P(("rep", "fs"), None), P("tp", "fs"), P("tp")),
        check_vma=False,
    )
```
